512 devices in a mesh: ep: 128 (over z, x, core), tp: 4 (over y).
Axes of the slice: x: 4, y: 4, z: 16, core: 2. Of those that a mesh axis runs over, the one named last changes fastest.
Arguments:
- tokens: bfloat16 [1536, 1024], P('ep'), may hold values from -6 to 6
- norm_gain: float32 [1024], replicated, may hold values from 0.1 to 1.9
- w_query: bfloat16 [1024, 512], P(None, 'tp'), may hold values from -0.1875 to 0.1875
- w_key: bfloat16 [1024, 512], P(None, 'tp'), may hold values from -0.1875 to 0.1875
- w_value: bfloat16 [1024, 512], P(None, 'tp'), may hold values from -0.1875 to 0.1875
- w_input_gate: bfloat16 [1024, 4], replicated, may hold values from -0.1875 to 0.1875
- w_forget_gate: bfloat16 [1024, 4], replicated, may hold values from -0.1875 to 0.1875
- input_bias: float32 [4], replicated, may hold values from -2 to 1
- forget_bias: float32 [4], replicated, may hold values from 0 to 4
- state_c: float32 [1536, 4, 128, 128], P('ep', 'tp'), may hold values from -1.75 to 1.75
- state_n: float32 [1536, 4, 128], P('ep', 'tp'), may hold values from -1.75 to 1.75
- state_m: float32 [1536, 4], P('ep', 'tp'), may hold values from -1 to 2
- w_mixer_out: bfloat16 [512, 1024], P('tp'), may hold values from -0.25 to 0.25
- ffn_gain: float32 [1024], replicated, may hold values from 0.1 to 1.9
- routes: int32 [1536, 6], P('ep'), may hold values from 0 to 127, all different within a row; in each aligned block of 12 rows (0 to 11, 12 to 23, ...) at most 2 rows name the same one
- route_scale: bfloat16 [1536, 6], P('ep'), may hold values from 0.099609375 to 1
- w_expert_gate: bfloat16 [128, 1024, 1024], P('ep', None, 'tp'), may hold values from -0.375 to 0.375
- w_expert_up: bfloat16 [128, 1024, 1024], P('ep', None, 'tp'), may hold values from -0.375 to 0.375
- w_expert_down: bfloat16 [128, 1024, 1024], P('ep', 'tp'), may hold values from -0.1875 to 0.1875
- w_dense_gate: bfloat16 [1024, 512], P(None, 'tp'), may hold values from -0.1875 to 0.1875
- w_dense_up: bfloat16 [1024, 512], P(None, 'tp'), may hold values from -0.1875 to 0.1875
- w_dense_down: bfloat16 [512, 1024], P('tp'), may hold values from -0.5 to 0.5
- w_branch_gate: bfloat16 [1024], replicated, may hold values from -0.1875 to 0.1875
Outputs:
- output: bfloat16 [1536, 1024], P('ep', 'tp')
- new_c: float32 [1536, 4, 128, 128], P('ep', 'tp')
- new_n: float32 [1536, 4, 128], P('ep', 'tp')
- new_m: float32 [1536, 4], P('ep', 'tp')
The draws below stay inside these ranges and needn't reach their ends.
Inputs may be any that keep to these rules, and one draw needn't show every extreme that they name: `routes`: each row names 6 different experts. Among the rows of one index of ep no expert is named by more than 2 rows, a bound that some block reaches of them.
All inputs are finite; a program needn't handle non-finite values.
Results may differ from the reference program's by a relative error of at most 0.018.
Values may be sent and summed in bfloat16 or wider, within the bound.
A program may use at most 64 MiB of HBM per device.

```python
import math
import jax
import jax.numpy as jnp
import numpy as np
from jax import lax

D = 1024
HEADS = 4
DQK = 128
DV = 128
D_EXPERT = 1024
DENSE_FF = 512
TOP_K = 6
SEQ_DEV = 12
EXPERTS = 128
TOKENS = 1536
CAP = 2
N_TP = 4


def block_scale(rng, dims, split, low, top_value):
    gain = 1.0
    for dim, parts in split:
        draws = jax.random.uniform(jax.random.fold_in(jax.random.fold_in(rng, 6), dim), (parts,), jnp.float32, low / len(split), top_value / len(split))
        gain = gain * jnp.repeat(jnp.exp(draws), dims[dim] // parts).reshape((-1,) + (1,) * (len(dims) - 1 - dim))
    return gain


def assign_block(rng, own, number, rows, count, top, most, slope):
    sequence = jax.random.permutation(rng, count)
    crowded, common = shares(count, rows * top, most, slope, True), shares(count, rows * top, most, slope, False)
    places = jnp.arange(count)

    def named(sizes, turn):
        used = int((sizes > 0).sum())
        fixed = max(1, used // 4)
        moved = fixed + (places - fixed + turn * (used - fixed)) % max(1, count - fixed)
        return jnp.zeros((count,), jnp.int32).at[sequence[jnp.where(places < fixed, places, moved)]].set(jnp.asarray(sizes, jnp.int32))

    sizes = jnp.where(number % 4 == 0, named(crowded, number // 4), named(common, number - number // 4 - 1))
    mixed = jax.random.permutation(jax.random.fold_in(own, 3), count)
    donor, taker = mixed[0:count // 2 * 2:2], mixed[1:count // 2 * 2:2]
    room = jnp.minimum(sizes[donor] - 1, most - sizes[taker]) // 2
    room = jnp.where((donor == sequence[0]) | (taker == sequence[0]) | (sizes[taker] == 0), 0, jnp.maximum(room, 0))
    moved = jax.random.randint(jax.random.fold_in(own, 4), (count // 2,), 0, 1 << 20) % (room + 1)
    sizes = sizes.at[donor].add(-moved).at[taker].add(moved)
    members = jnp.searchsorted(jnp.cumsum(sizes), jnp.arange(rows * top), side="right").astype(jnp.int32)
    listing = members.reshape(top, rows).T
    listing = listing[jax.random.permutation(jax.random.fold_in(own, 1), rows)]
    turn = jax.random.randint(jax.random.fold_in(own, 2), (rows, 1), 0, top)
    return jnp.take_along_axis(listing, (jnp.arange(top)[None, :] + turn) % top, axis=1)


def shares(number_of, total, most, lean, full):
    weights = [(1 << 20) // math.isqrt(standing ** lean) + 1 for standing in range(1, number_of + 1)]
    largest = most if full else min(most, max(-(-total // number_of), total * weights[0] // sum(weights)))
    least = 1 if total - largest >= number_of - 1 else 0
    given, surplus = [largest] + [least] * (number_of - 1), total - largest - least * (number_of - 1)
    while surplus > 0:
        free = [i for i in range(1, number_of) if given[i] < largest] or [i for i in range(1, number_of) if given[i] < most]
        whole, left = sum([weights[i] for i in free]), surplus
        for i in free:
            extra = min(most - given[i], max(1, left * weights[i] // whole), surplus)
            given[i] = given[i] + extra
            surplus = surplus - extra
    return np.array(given)


def scatter_about(own_key, shape, spread, limit, pieces=(), kind=jnp.bfloat16):
    array = jax.random.normal(own_key, shape, jnp.float32) * spread
    if len(pieces) > 0:
        array = block_scale(own_key, shape, pieces, -0.22, 0.18) * array
    return jnp.clip(array, min=-limit, max=limit).astype(kind)


def setup_inputs(seed: int = 0) -> dict:
    key_list = jax.random.split(jax.random.key(seed), 24)
    tokens = scatter_about(key_list[0], (TOKENS, D), 1.0, 6.0, ((0, 128),))
    norm_gain = jnp.clip(1.0 + 0.18 * jax.random.normal(key_list[1], (D,), jnp.float32), 0.1, 1.9)
    w_query = scatter_about(key_list[2], (D, HEADS * DQK), D ** -0.5, 0.1875, ((1, 4),))
    w_key = scatter_about(key_list[3], (D, HEADS * DQK), D ** -0.5, 0.1875, ((1, 4),))
    w_value = scatter_about(key_list[4], (D, HEADS * DV), D ** -0.5, 0.1875, ((1, 4),))
    w_input_gate = scatter_about(key_list[5], (D, HEADS), D ** -0.5, 0.1875)
    w_forget_gate = scatter_about(key_list[6], (D, HEADS), D ** -0.5, 0.1875)
    input_bias = jnp.clip(jax.random.uniform(key_list[7], (HEADS,), jnp.float32, -2.0, 1.0), -2.0, 1.0)
    forget_bias = jnp.clip(jax.random.uniform(key_list[8], (HEADS,), jnp.float32, 0.0, 4.0), 0.0, 4.0)
    state_c = scatter_about(key_list[9], (TOKENS, HEADS, DQK, DV), 0.3, 1.75, ((0, 128), (1, 4)), jnp.float32)
    state_n = scatter_about(key_list[10], (TOKENS, HEADS, DQK), 0.3, 1.75, ((0, 128), (1, 4)), jnp.float32)
    state_m = jnp.clip(-1.0 + 3.0 * jax.random.uniform(key_list[11], (TOKENS, HEADS), jnp.float32) ** block_scale(key_list[11], (TOKENS, HEADS), ((0, 128), (1, 4)), -0.2, 0.2), -1.0, 2.0)
    w_mixer_out = scatter_about(key_list[12], (HEADS * DV, D), (HEADS * DV) ** -0.5, 0.25, ((0, 4),))
    ffn_gain = jnp.clip(1.0 + 0.18 * jax.random.normal(key_list[13], (D,), jnp.float32), 0.1, 1.9)
    routes_keys = jax.random.split(jax.random.fold_in(key_list[14], 1), TOKENS // SEQ_DEV)
    routes_turns = jax.random.permutation(jax.random.fold_in(key_list[14], 3), TOKENS // SEQ_DEV)
    routes = jax.vmap(lambda own, number: assign_block(jax.random.fold_in(key_list[14], 2), own, number, SEQ_DEV, EXPERTS, TOP_K, CAP, 2))(routes_keys, routes_turns).reshape((TOKENS, TOP_K))
    route_scale = jnp.clip(jnp.exp(math.log(1.0) - 2.306499 * jax.random.uniform(key_list[15], (TOKENS, TOP_K), jnp.float32) ** block_scale(key_list[15], (TOKENS, TOP_K), ((0, 128),), -0.2, 0.2)), 0.099609375, 1.0).astype(jnp.bfloat16)
    w_expert_gate = scatter_about(key_list[16], (EXPERTS, D, D_EXPERT), (2.0 * D ** -0.5), 0.375, ((0, 128), (2, 4)))
    w_expert_up = scatter_about(key_list[17], (EXPERTS, D, D_EXPERT), (2.0 * D ** -0.5), 0.375, ((0, 128), (2, 4)))
    w_expert_down = scatter_about(key_list[18], (EXPERTS, D_EXPERT, D), D_EXPERT ** -0.5, 0.1875, ((0, 128), (1, 4)))
    w_dense_gate = scatter_about(key_list[19], (D, DENSE_FF), D ** -0.5, 0.1875, ((1, 4),))
    w_dense_up = scatter_about(key_list[20], (D, DENSE_FF), D ** -0.5, 0.1875, ((1, 4),))
    w_dense_down = scatter_about(key_list[21], (DENSE_FF, D), (DENSE_FF // 4) ** -0.5, 0.5, ((0, 4),))
    w_branch_gate = scatter_about(key_list[22], (D,), D ** -0.5, 0.1875)
    return {"tokens": tokens, "norm_gain": norm_gain, "w_query": w_query, "w_key": w_key, "w_value": w_value, "w_input_gate": w_input_gate, "w_forget_gate": w_forget_gate, "input_bias": input_bias, "forget_bias": forget_bias, "state_c": state_c, "state_n": state_n, "state_m": state_m, "w_mixer_out": w_mixer_out, "ffn_gain": ffn_gain, "routes": routes, "route_scale": route_scale, "w_expert_gate": w_expert_gate, "w_expert_up": w_expert_up, "w_expert_down": w_expert_down, "w_dense_gate": w_dense_gate, "w_dense_up": w_dense_up, "w_dense_down": w_dense_down, "w_branch_gate": w_branch_gate}


EPSILON = 1e-06
CLAMP_LIMIT = 7.0
SWISH_ALPHA = 1.702

def stored(values):
    return lax.optimization_barrier(values.astype(jnp.bfloat16)).astype(jnp.float32)

def rms_scaled(values, gain_vec):
    values = values.astype(jnp.float32)
    scaled = values * lax.rsqrt(lax.optimization_barrier(jnp.mean(values * values, axis=-1, keepdims=True)) + EPSILON)
    return scaled * gain_vec.astype(jnp.float32)

def slot_tables(route_blocks, expert_ids, weight_blocks, capacity, top_count):
    entries = route_blocks.shape[1]
    matched = (route_blocks[:, None, :] == expert_ids[None, :, None]).astype(jnp.int32)
    ranking = jnp.cumsum(matched, axis=2, dtype=jnp.int32) - 1
    slot_ids = jnp.arange(capacity, dtype=jnp.int32)
    chosen = (matched[:, :, None, :] == 1) & (ranking[:, :, None, :] == slot_ids[None, None, :, None])
    slot_hot = jnp.where(chosen, 1.0, 0.0).astype(jnp.float32)
    entry_ids = jnp.arange(entries, dtype=jnp.int32)
    token_ids = jnp.arange(entries // top_count, dtype=jnp.int32)
    owner = jnp.where(entry_ids[:, None] // top_count == token_ids[None, :], 1.0, 0.0).astype(jnp.float32)
    token_hot = jnp.einsum('becj,js->becs', slot_hot, owner, precision=lax.Precision.HIGHEST)
    slot_weight = jnp.einsum('becj,bj->bec', slot_hot, weight_blocks, precision=lax.Precision.HIGHEST)
    return (token_hot, slot_weight)

def reference(tokens, norm_gain, w_query, w_key, w_value, w_input_gate, w_forget_gate, input_bias, forget_bias, state_c, state_n, state_m, w_mixer_out, ffn_gain, routes, route_scale, w_expert_gate, w_expert_up, w_expert_down, w_dense_gate, w_dense_up, w_dense_down, w_branch_gate):
    row_count = tokens.shape[0]
    normed = rms_scaled(tokens, norm_gain).astype(jnp.bfloat16)
    queries = stored(jnp.dot(normed, w_query, preferred_element_type=jnp.float32)).reshape(row_count, HEADS, DQK)
    key_rows = stored(jnp.dot(normed, w_key, preferred_element_type=jnp.float32)).reshape(row_count, HEADS, DQK)
    value_rows = stored(jnp.dot(normed, w_value, preferred_element_type=jnp.float32)).reshape(row_count, HEADS, DV)
    input_pre = jnp.dot(normed, w_input_gate, preferred_element_type=jnp.float32) + input_bias
    forget_log = jax.nn.log_sigmoid(jnp.dot(normed, w_forget_gate, preferred_element_type=jnp.float32) + forget_bias)
    new_m = jnp.maximum(forget_log + state_m, input_pre)
    forget_factor = jnp.exp(forget_log + state_m - new_m)
    input_factor = jnp.exp(input_pre - new_m)
    key_scaled = key_rows * DQK ** (-0.5)
    new_c = forget_factor[..., None, None] * state_c + input_factor[..., None, None] * (key_scaled[..., :, None] * value_rows[..., None, :])
    new_n = forget_factor[..., None] * state_n + input_factor[..., None] * key_scaled
    numer = jnp.einsum('thd,thdv->thv', queries, new_c, precision=lax.Precision.HIGHEST)
    denom = jnp.einsum('thd,thd->th', queries, new_n, precision=lax.Precision.HIGHEST)
    head_out = (numer / jnp.maximum(jnp.abs(denom), 1.0)[..., None]).astype(jnp.bfloat16).reshape(row_count, HEADS * DV)
    group_width = HEADS // N_TP * DV
    mixer_total = jnp.zeros((row_count, D), jnp.float32)
    for group in range(N_TP):
        lower = group * group_width
        mixer_total = mixer_total + stored(jnp.dot(head_out[:, lower:lower + group_width], w_mixer_out[lower:lower + group_width], preferred_element_type=jnp.float32))
    mixer_out = mixer_total.astype(jnp.bfloat16)
    residual = tokens.astype(jnp.float32) + mixer_out.astype(jnp.float32)
    ffn_in = rms_scaled(residual, ffn_gain).astype(jnp.bfloat16)
    scale_values = route_scale.astype(jnp.float32)
    route_weight = scale_values / lax.optimization_barrier(jnp.sum(scale_values, axis=1, keepdims=True))
    block_count = row_count // SEQ_DEV
    route_blocks = routes.reshape(block_count, SEQ_DEV * TOP_K)
    weight_blocks = route_weight.reshape(block_count, SEQ_DEV * TOP_K)
    token_blocks = ffn_in.astype(jnp.float32).reshape(block_count, SEQ_DEV, D)
    part_width = D_EXPERT // N_TP

    def one_expert(total, inputs):
        gate_weight, up_weight, down_weight, expert = inputs
        token_hot, slot_weight = slot_tables(route_blocks, expert[None], weight_blocks, CAP, TOP_K)
        token_hot = token_hot[:, 0]
        slot_weight = slot_weight[:, 0]
        slot_rows = jnp.einsum('bcs,bsd->bcd', token_hot, token_blocks, precision=lax.Precision.HIGHEST).astype(jnp.bfloat16).reshape(block_count * CAP, D)
        gate_pre = jnp.minimum(jnp.dot(slot_rows, gate_weight, preferred_element_type=jnp.float32), CLAMP_LIMIT)
        up_pre = jnp.clip(jnp.dot(slot_rows, up_weight, preferred_element_type=jnp.float32), -CLAMP_LIMIT, CLAMP_LIMIT)
        hidden = (gate_pre * jax.nn.sigmoid(SWISH_ALPHA * gate_pre) * (up_pre + 1.0)).astype(jnp.bfloat16)
        expert_out = jnp.zeros((block_count * CAP, D), jnp.float32)
        for part in range(N_TP):
            lower = part * part_width
            expert_out = expert_out + stored(jnp.dot(hidden[:, lower:lower + part_width], down_weight[lower:lower + part_width], preferred_element_type=jnp.float32))
        weighted = expert_out.reshape(block_count, CAP, D) * slot_weight[..., None]
        total = total + jnp.einsum('bcs,bcd->bsd', token_hot, weighted, precision=lax.Precision.HIGHEST)
        return (total, None)
    moe, _ = lax.scan(one_expert, jnp.zeros((block_count, SEQ_DEV, D), jnp.float32), (w_expert_gate, w_expert_up, w_expert_down, jnp.arange(EXPERTS, dtype=jnp.int32)))
    dense_gate_pre = jnp.dot(ffn_in, w_dense_gate, preferred_element_type=jnp.float32)
    dense_hidden = (jax.nn.silu(dense_gate_pre) * jnp.dot(ffn_in, w_dense_up, preferred_element_type=jnp.float32)).astype(jnp.bfloat16)
    dense = jnp.dot(dense_hidden, w_dense_down, preferred_element_type=jnp.float32)
    branch_weight = jax.nn.sigmoid(jnp.dot(ffn_in, w_branch_gate, preferred_element_type=jnp.float32))
    output = (residual + moe.reshape(row_count, D) + branch_weight[:, None] * dense).astype(jnp.bfloat16)
    return (output, new_c, new_n, new_m)
```

```python
import jax
import jax.numpy as jnp
from jax import lax
from jax.experimental import pallas as pl
from jax.experimental.pallas import tpu as pltpu
from jax.sharding import PartitionSpec as P

EPSILON = 1e-06
CLAMP_LIMIT = 7.0
SWISH_ALPHA = 1.702

F32 = jnp.float32
BF16 = jnp.bfloat16
MESH = pl.DeviceIdType.MESH

NZ, NX, NC, NY = 16, 4, 2, 4
PLANE = NX * NC
ROWS, WIDTH, HEAD, TOP = 12, 1024, 128, 6
QUARTER = WIDTH // NY
STACK = 2 * ROWS
PITCH = 32
GROUP = 4
CHUNKS = NZ // GROUP
SLOTS = 2 * GROUP
SERVED = PLANE * SLOTS
ALL = NY * SERVED
ORDER = (0, 1, 15, 2, 14, 3, 13, 4, 12, 5, 11, 6, 10, 7, 9, 8)
PLACES = tuple(reversed(range(1, NZ)))
Y_ORDER = (2, 1, 3)
PLANE_ORDER = tuple(
    (dx, dc, dy) for dy in (2, 1, 3, 0) for dx in (2, 1, 3, 0) for dc in (1, 0) if dx + dc + dy
)
STEPS = "z3 z2 z1 z0 dense x3 x2 x1 x0 b3 b2 b1 b0".split()


def dot(a, b):
    return jnp.dot(a, b, preferred_element_type=F32)


def dot_rows(a, b):
    return lax.dot_general(a, b, (((1,), (1,)), ((), ())), preferred_element_type=F32)


def dot_columns(a, b):
    return lax.dot_general(a, b, (((0,), (0,)), ((), ())), preferred_element_type=F32)


def layer_kernel(
    tok_h,
    norm_gain_h,
    wq_h,
    wk_h,
    wv_h,
    wig_h,
    wfg_h,
    ibias_h,
    fbias_h,
    c_h,
    n_h,
    m_h,
    wmix_h,
    ffn_gain_h,
    routes_h,
    scales_h,
    weg_h,
    weu_h,
    wed_h,
    wdg_h,
    wdu_h,
    wdd_h,
    wbg_h,
    out,
    newc,
    newn,
    newm,
    tok,
    norm_gain,
    wq,
    wk,
    wv,
    wig,
    wfg,
    ibias,
    fbias,
    cst,
    n_in,
    m_in,
    wmix,
    ffn_gain,
    routes,
    scales,
    weg,
    weu,
    wed,
    wdg,
    wdu,
    wdd,
    wbg,
    kq,
    num,
    meta,
    meta_tile,
    meta_all,
    part,
    part_all,
    res_all,
    own_row,
    wide,
    stack,
    zbuf,
    hot,
    slot_weight,
    sbuf,
    xbuf,
    obuf,
    rbuf,
    backz,
    rz,
    dsend,
    drecv,
    local_sem,
    part_s,
    part_r,
    res_s,
    res_r,
    meta_s,
    meta_r,
    z_s,
    z_r,
    x_s,
    x_r,
    d_s,
    d_r,
    b_s,
    b_r,
    w_s,
    w_r,
):
    ep = lax.axis_index("ep")
    y = lax.axis_index("tp")
    z = ep // PLANE
    g = ep % PLANE
    x = g // NC
    c = g % NC

    def z_peer(d):
        return (((z + d) % NZ) * PLANE + g, y)

    def y_peer(d):
        return (ep, (y + d) % NY)

    def plane_peer(dx, dc, dy):
        plane = ((x + dx + NX) % NX) * NC + (c + dc + NC) % NC
        return (z * PLANE + plane, (y + dy + NY) % NY)

    def columns(d):
        return pl.ds(pl.multiple_of(((y + d + NY) % NY) * QUARTER, QUARTER), QUARTER)

    def remote(src, dst, send, recv, peer):
        return pltpu.make_async_remote_copy(
            src_ref=src, dst_ref=dst, send_sem=send, recv_sem=recv, device_id=peer, device_id_type=MESH
        )

    loads = {}
    for number, (name, src, dst) in enumerate(
        (
            ("tok", tok_h, tok),
            ("ng", norm_gain_h, norm_gain),
            ("q", wq_h, wq),
            ("k", wk_h, wk),
            ("v", wv_h, wv),
            ("ig", wig_h, wig),
            ("fg", wfg_h, wfg),
            ("ib", ibias_h, ibias),
            ("fb", fbias_h, fbias),
            ("m", m_h, m_in),
            ("n", n_h, n_in),
            ("routes", routes_h, routes),
            ("scales", scales_h, scales),
            ("c", c_h, cst),
            ("mix", wmix_h, wmix),
            ("gain", ffn_gain_h, ffn_gain),
            ("bg", wbg_h, wbg),
            ("dg", wdg_h, wdg),
            ("du", wdu_h, wdu),
            ("dd", wdd_h, wdd),
            ("eg", weg_h, weg),
            ("eu", weu_h, weu),
            ("ed", wed_h, wed),
        )
    ):
        loads[name] = pltpu.make_async_copy(src, dst, local_sem.at[number])
        loads[name].start()

    zbuf[...] = jnp.zeros_like(zbuf)
    barrier = pltpu.get_barrier_semaphore()
    for p in PLACES:
        pl.semaphore_signal(barrier, inc=1, device_id=z_peer(ORDER[p]), device_id_type=MESH)
    for place in PLANE_ORDER:
        pl.semaphore_signal(barrier, inc=1, device_id=plane_peer(*place), device_id_type=MESH)

    kq[...] = jnp.zeros_like(kq)
    meta[...] = jnp.zeros_like(meta)

    loads["tok"].wait()
    loads["ng"].wait()
    tokens = tok[...].astype(F32)
    mean = jnp.mean(tokens * tokens, axis=-1, keepdims=True)
    normed = (tokens * lax.rsqrt(mean + EPSILON) * norm_gain[...]).astype(BF16)
    loads["q"].wait()
    query = dot(normed, wq[...]).astype(BF16).astype(F32)
    loads["k"].wait()
    key_scaled = dot(normed, wk[...]).astype(BF16).astype(F32) * HEAD ** (-0.5)
    loads["v"].wait()
    value = dot(normed, wv[...]).astype(BF16).astype(F32)
    loads["ig"].wait()
    loads["fg"].wait()
    head = lax.broadcasted_iota(jnp.int32, (NY, ROWS), 0) == y
    input_all = dot_rows(wig[...], normed)
    forget_all = dot_rows(wfg[...], normed)
    for name in ("ib", "fb", "m", "n"):
        loads[name].wait()
    input_pre = jnp.sum(jnp.where(head, input_all, 0.0), axis=0, keepdims=True) + ibias[y]
    forget_pre = jnp.sum(jnp.where(head, forget_all, 0.0), axis=0, keepdims=True) + fbias[y]
    forget_log = jnp.minimum(forget_pre, 0.0) - jnp.log1p(jnp.exp(-jnp.abs(forget_pre)))
    state_m = m_in[...]
    new_m = jnp.maximum(forget_log + state_m, input_pre)
    forget = jnp.exp(forget_log + state_m - new_m)
    entry = jnp.exp(input_pre - new_m)
    newm[...] = new_m
    same = lax.broadcasted_iota(jnp.int32, (ROWS, ROWS), 0) == lax.broadcasted_iota(
        jnp.int32, (ROWS, ROWS), 1
    )
    forget_col = jnp.sum(jnp.where(same, forget, 0.0), axis=1, keepdims=True)
    entry_col = jnp.sum(jnp.where(same, entry, 0.0), axis=1, keepdims=True)
    key_in = key_scaled * entry_col
    new_n = forget_col * n_in[:, 0, :] + key_in
    newn[:, 0, :] = new_n
    denom = jnp.sum(query * new_n, axis=1, keepdims=True)
    both = jnp.sum(query * key_in, axis=1, keepdims=True)
    kq[0:ROWS, :] = key_in
    kq[16 : 16 + ROWS, :] = query
    turned = kq[...].T
    loads["c"].wait()
    for t in range(ROWS):
        num[t : t + 1, :] = jnp.sum(turned[:, 16 + t : 17 + t] * cst[t], axis=0, keepdims=True)
    numer = forget_col * num[...] + both * value
    head_out = (numer / jnp.maximum(jnp.abs(denom), 1.0)).astype(BF16)
    loads["mix"].wait()
    mixed = dot(head_out, wmix[...])
    wide[...] = mixed
    for d in range(NY):
        part[d] = wide[:, columns(d)].astype(BF16)

    loads["routes"].wait()
    loads["scales"].wait()
    meta[0:TOP, 0:ROWS] = routes[...].astype(F32) + 1.0
    table = meta[...]
    table = table + pltpu.roll(table, ROWS, 1)
    meta[0:TOP, 0:ROWS] = scales[...].astype(F32)
    scale_table = meta[...]
    scale_table = scale_table + pltpu.roll(scale_table, ROWS, 1)
    meta_tile[...] = (table + pltpu.roll(scale_table, PITCH, 1)).astype(BF16)

    pl.semaphore_wait(barrier, NZ - 1 + len(PLANE_ORDER))

    for k, d in enumerate(Y_ORDER):
        remote(part.at[d], part_all.at[k], part_s, part_r, y_peer(d)).start()
    for p in PLACES:
        remote(meta_tile, meta_all.at[p], meta_s, meta_r, z_peer(ORDER[p])).start()

    def every(ref, send, recv):
        return remote(ref, ref, send, recv, y_peer(1))

    part_done = every(part_all, part_s, part_r)
    meta_done = every(meta_all.at[1:NZ], meta_s, meta_r)

    for t in range(ROWS):
        newc[t] = forget[0:1, t : t + 1] * cst[t] + turned[:, t : t + 1] * value[t : t + 1, :]
    wide[...] = tokens
    tokens_own = wide[:, columns(0)]

    part_done.wait_recv()
    mixer = part[0].astype(F32)
    for k in range(NY - 1):
        mixer = mixer + part_all[k].astype(F32)
    residual = tokens_own + mixer.astype(BF16).astype(F32)
    stack[0:ROWS, :] = residual[:, :HEAD]
    stack[ROWS:STACK, :] = residual[:, HEAD:]
    zbuf[0, 0:STACK, :] = stack[...].astype(BF16)
    for p in PLACES:
        remote(
            zbuf.at[0, 0:STACK],
            zbuf.at[p, 0:STACK],
            z_s,
            z_r.at[p // GROUP],
            z_peer(ORDER[p]),
        ).start()
    own_row[...] = residual.astype(BF16)
    for d in Y_ORDER:
        remote(own_row, res_all.at[d - 1], res_s, res_r, y_peer(d)).start()
    res_done = every(res_all, res_s, res_r)

    meta_done.wait_recv()
    meta_all[0] = meta_tile[...]
    lane = lax.broadcasted_iota(jnp.int32, (PLANE, HEAD), 1)
    spot = lane & (PITCH - 1)
    position = jnp.where(spot >= ROWS, spot - ROWS, spot)
    relative = lax.broadcasted_iota(jnp.int32, (PLANE, HEAD), 0)
    expert = z * PLANE + ((x + (relative >> 1)) & (NX - 1)) * NC + ((c + relative) & (NC - 1))
    expert = (expert + 1).astype(F32)
    slot = lax.broadcasted_iota(jnp.int32, (SLOTS, HEAD), 0)
    slot_lane = lax.broadcasted_iota(jnp.int32, (SLOTS, HEAD), 1)
    offset = slot_lane - PITCH * (slot >> 1)
    turns = []
    for h in range(2):
        base = (offset >= ROWS * h) & (offset < ROWS * (h + 1))
        turns.append(jnp.where(base, (slot & 1).astype(F32), 9.0))
    for k in range(CHUNKS):
        named_by = jnp.zeros((PLANE, HEAD), F32)
        scale_by = jnp.zeros((PLANE, HEAD), F32)
        for i in range(GROUP):
            tile = meta_all[k * GROUP + i].astype(F32)
            first = jnp.where(lane < PITCH, tile, 0.0)
            second = tile - first
            named_by = named_by + (pltpu.roll(first, PITCH * i, 1) if i else first)
            scale_by = scale_by + (
                pltpu.roll(second, PITCH * (i - 1) % HEAD, 1) if i != 1 else second
            )
        scale_sum = jnp.sum(scale_by[0:TOP], axis=0, keepdims=True)
        scale_sum = jnp.where(scale_sum > 0.0, scale_sum, 1.0)
        named = jnp.zeros((PLANE, HEAD), F32)
        weight = jnp.zeros((PLANE, HEAD), F32)
        for j in range(TOP):
            hit = named_by[j : j + 1, :] == expert
            named = jnp.where(hit, 1.0, named)
            weight = jnp.where(hit, scale_by[j : j + 1, :] / scale_sum, weight)
        seen = named
        for d in (1, 2, 4, 8):
            seen = jnp.maximum(seen, jnp.where(position >= d, pltpu.roll(seen, d, 1), 0.0))
        earlier = jnp.where(position >= 1, pltpu.roll(seen, 1, 1), 0.0)
        rank = jnp.where(named > 0, earlier, 5.0)
        pieces = []
        weights = []
        for h in range(2):
            for e in range(PLANE):
                chosen = rank[e : e + 1, :] == turns[h]
                pieces.append(jnp.where(chosen, 1.0, 0.0))
                if h == 0:
                    weights.append(
                        jnp.sum(
                            jnp.where(chosen, weight[e : e + 1, :], 0.0), axis=1, keepdims=True
                        )
                    )
        hot[k] = jnp.concatenate(pieces, axis=0).astype(BF16)
        slot_weight[k] = jnp.concatenate(weights, axis=0)

    def z_step(k):
        there = zbuf.at[max(1, k * GROUP) : (k + 1) * GROUP, 0:STACK]
        every(there, z_s, z_r.at[k]).wait_recv()
        slots = dot(hot[k], zbuf[k * GROUP : (k + 1) * GROUP].reshape(HEAD, HEAD))
        sbuf[k, :, 0:HEAD] = slots[0:SERVED].astype(BF16)
        sbuf[k, :, HEAD:] = slots[SERVED:].astype(BF16)
        for dx, dc, dy in PLANE_ORDER:
            r = (dx * NC + dc) * SLOTS
            to = dy * SERVED + r
            remote(
                sbuf.at[k, r : r + SLOTS],
                xbuf.at[k, to : to + SLOTS],
                x_s,
                x_r.at[k],
                plane_peer(dx, dc, dy),
            ).start()
        xbuf[k, 0:SLOTS, :] = sbuf[k, 0:SLOTS, :]

    def x_step(k):
        if "eg" in loads:
            for name in ("eg", "eu", "ed"):
                loads.pop(name).wait()
        every(xbuf.at[k, SLOTS:ALL], x_s, x_r.at[k]).wait_recv()
        squares = jnp.zeros((SERVED, 1), F32)
        for d in range(NY):
            rows = xbuf[k, d * SERVED : (d + 1) * SERVED, :].astype(F32)
            squares = squares + jnp.sum(rows * rows, axis=1, keepdims=True)
        scale = lax.rsqrt(squares * (1.0 / WIDTH) + EPSILON)
        gate = jnp.zeros((SERVED, QUARTER), F32)
        up = jnp.zeros((SERVED, QUARTER), F32)
        for d in range(NY):
            rows = xbuf[k, d * SERVED : (d + 1) * SERVED, :].astype(F32)
            rows = (rows * scale * ffn_gain[:, columns(-d)]).astype(BF16)
            gate = gate + dot(rows, weg[columns(-d), :])
            up = up + dot(rows, weu[columns(-d), :])
        gate = jnp.minimum(gate, CLAMP_LIMIT)
        up = jnp.clip(up, -CLAMP_LIMIT, CLAMP_LIMIT)
        hidden = (gate * jax.nn.sigmoid(SWISH_ALPHA * gate) * (up + 1.0)).astype(BF16)
        for d in range(NY):
            obuf[k, d * SERVED : (d + 1) * SERVED, :] = dot(hidden, wed[:, columns(d)]).astype(
                BF16
            )
        for dx, dc, dy in PLANE_ORDER:
            r = dy * SERVED + (dx * NC + dc) * SLOTS
            remote(
                obuf.at[k, r : r + SLOTS],
                rbuf.at[k, r : r + SLOTS],
                b_s,
                b_r.at[k],
                plane_peer(-dx, -dc, dy),
            ).start()
        rbuf[k, 0:SLOTS, :] = obuf[k, 0:SLOTS, :]

    def b_step(k):
        every(rbuf.at[k, SLOTS:ALL], b_s, b_r.at[k]).wait_recv()
        total = rbuf[k, 0:SERVED, :].astype(F32)
        for d in range(1, NY):
            total = total + rbuf[k, d * SERVED : (d + 1) * SERVED, :].astype(F32)
        served = (total * slot_weight[k]).astype(BF16)
        combined = dot_columns(hot[k, 0:SERVED, :], served[:, :HEAD]) + dot_columns(
            hot[k, SERVED:, :], served[:, HEAD:]
        )
        backz[k * GROUP : (k + 1) * GROUP] = combined.reshape(GROUP, PITCH, HEAD).astype(BF16)
        for p in reversed(range(k * GROUP, (k + 1) * GROUP)):
            if p:
                remote(
                    backz.at[p, 0:STACK], rz.at[p, 0:STACK], w_s, w_r, z_peer(NZ - ORDER[p])
                ).start()

    def dense_step():
        res_done.wait_recv()
        wide[:, columns(0)] = own_row[...].astype(F32)
        for d in Y_ORDER:
            wide[:, columns(-d)] = res_all[d - 1].astype(F32)
        whole_row = wide[...]
        mean = jnp.mean(whole_row * whole_row, axis=-1, keepdims=True)
        ffn_in = (whole_row * lax.rsqrt(mean + EPSILON) * ffn_gain[...]).astype(BF16)
        ffn_wide = ffn_in.astype(F32)
        for name in ("bg", "dg", "du", "dd"):
            loads[name].wait()
        gate = dot(ffn_in, wdg[...])
        dense_hidden = (gate * jax.nn.sigmoid(gate) * dot(ffn_in, wdu[...])).astype(BF16)
        branch = jnp.zeros((ROWS, HEAD), F32)
        gate_row = wbg[...].astype(F32)
        for k in range(WIDTH // HEAD):
            branch = branch + ffn_wide[:, k * HEAD : (k + 1) * HEAD] * gate_row[k : k + 1, :]
        branch = jax.nn.sigmoid(jnp.sum(branch, axis=1, keepdims=True))
        wide[...] = dot(dense_hidden, wdd[...]) * branch
        for d in range(NY):
            dsend[d] = wide[:, columns(d)].astype(BF16)
        for k, d in enumerate(Y_ORDER):
            remote(dsend.at[d], drecv.at[k], d_s, d_r, y_peer(d)).start()

    for step in STEPS:
        if step == "dense":
            loads["gain"].wait()
            dense_step()
        else:
            {"z": z_step, "x": x_step, "b": b_step}[step[0]](int(step[1]))

    every(drecv, d_s, d_r).wait()
    dense = dsend[0].astype(F32)
    for k in range(NY - 1):
        dense = dense + drecv[k].astype(F32)
    dense = residual + dense
    moe = backz[0, 0:STACK, :].astype(F32)
    part_done.wait_send()
    meta_done.wait_send()
    res_done.wait_send()
    every(zbuf.at[1:NZ, 0:STACK], z_s, z_r.at[0]).wait_send()
    every(xbuf.at[:, SLOTS:ALL], x_s, x_r.at[0]).wait_send()
    every(rbuf.at[:, SLOTS:ALL], b_s, b_r.at[0]).wait_send()
    w_done = every(rz.at[1:NZ, 0:STACK], w_s, w_r)
    w_done.wait()
    for p in range(1, NZ):
        moe = moe + rz[p, 0:STACK, :].astype(F32)
    stack[...] = moe
    moe = jnp.concatenate([stack[0:ROWS, :], stack[ROWS:STACK, :]], axis=1)
    out[...] = (dense + moe).astype(BF16)


def write_kernel(out, newc, newn, newm, out_h, newc_h, newn_h, newm_h, sem):
    copies = [
        pltpu.make_async_copy(src, dst, sem.at[k])
        for k, (src, dst) in enumerate(
            ((out, out_h), (newc, newc_h), (newn, newn_h), (newm, newm_h))
        )
    ]
    for copy in copies:
        copy.start()
    for copy in copies:
        copy.wait()


RESULTS = (
    ((ROWS, QUARTER), BF16),
    ((ROWS, HEAD, HEAD), F32),
    ((ROWS, 1, HEAD), F32),
    ((1, ROWS), F32),
)


def local(
    tokens,
    norm_gain,
    w_query,
    w_key,
    w_value,
    w_input_gate,
    w_forget_gate,
    input_bias,
    forget_bias,
    state_c,
    state_n,
    state_m,
    w_mixer_out,
    ffn_gain,
    routes,
    route_scale,
    w_expert_gate,
    w_expert_up,
    w_expert_down,
    w_dense_gate,
    w_dense_up,
    w_dense_down,
    w_branch_gate,
):
    vmem = pl.BlockSpec(memory_space=pltpu.VMEM)
    hbm = pl.BlockSpec(memory_space=pl.ANY)
    dma = pltpu.SemaphoreType.DMA
    operands = (
        tokens,
        norm_gain.reshape(1, WIDTH),
        w_query,
        w_key,
        w_value,
        w_input_gate.T,
        w_forget_gate.T,
        input_bias,
        forget_bias,
        state_c.reshape(ROWS, HEAD, HEAD),
        state_n,
        state_m.T,
        w_mixer_out,
        ffn_gain.reshape(1, WIDTH),
        routes.T,
        route_scale.T,
        w_expert_gate.reshape(WIDTH, QUARTER),
        w_expert_up.reshape(WIDTH, QUARTER),
        w_expert_down.reshape(QUARTER, WIDTH),
        w_dense_gate,
        w_dense_up,
        w_dense_down,
        w_branch_gate.reshape(WIDTH // HEAD, HEAD),
    )
    copies = [
        pltpu.SMEM(a.shape, a.dtype) if a.ndim == 1 else pltpu.VMEM(a.shape, a.dtype)
        for a in operands
    ]
    results = pl.pallas_call(
        layer_kernel,
        out_shape=tuple(pltpu.VMEM(shape, kind) for shape, kind in RESULTS),
        in_specs=[hbm] * len(operands),
        out_specs=(vmem,) * len(RESULTS),
        scratch_shapes=copies
        + [
            pltpu.VMEM((HEAD, HEAD), F32),
            pltpu.VMEM((ROWS, HEAD), F32),
            pltpu.VMEM((PLANE, HEAD), F32),
            pltpu.VMEM((PLANE, HEAD), BF16),
            pltpu.VMEM((NZ, PLANE, HEAD), BF16),
            pltpu.VMEM((NY, ROWS, QUARTER), BF16),
            pltpu.VMEM((NY - 1, ROWS, QUARTER), BF16),
            pltpu.VMEM((NY - 1, ROWS, QUARTER), BF16),
            pltpu.VMEM((ROWS, QUARTER), BF16),
            pltpu.VMEM((ROWS, WIDTH), F32),
            pltpu.VMEM((STACK, HEAD), F32),
            pltpu.VMEM((NZ, PITCH, HEAD), BF16),
            pltpu.VMEM((CHUNKS, 2 * SERVED, HEAD), BF16),
            pltpu.VMEM((CHUNKS, SERVED, 1), F32),
            pltpu.VMEM((CHUNKS, SERVED, QUARTER), BF16),
            pltpu.VMEM((CHUNKS, ALL, QUARTER), BF16),
            pltpu.VMEM((CHUNKS, ALL, QUARTER), BF16),
            pltpu.VMEM((CHUNKS, ALL, QUARTER), BF16),
            pltpu.VMEM((NZ, PITCH, HEAD), BF16),
            pltpu.VMEM((NZ, PITCH, HEAD), BF16),
            pltpu.VMEM((NY, ROWS, QUARTER), BF16),
            pltpu.VMEM((NY - 1, ROWS, QUARTER), BF16),
            dma((len(operands),)),
            dma(()),
            dma(()),
            dma(()),
            dma(()),
            dma(()),
            dma(()),
            dma(()),
            dma((CHUNKS,)),
            dma(()),
            dma((CHUNKS,)),
            dma(()),
            dma(()),
            dma(()),
            dma((CHUNKS,)),
            dma(()),
            dma(()),
        ],
        compiler_params=pltpu.CompilerParams(collective_id=0, has_side_effects=True),
    )(*operands)
    output, new_c, new_n, new_m = pl.pallas_call(
        write_kernel,
        out_shape=tuple(jax.ShapeDtypeStruct(shape, kind) for shape, kind in RESULTS),
        in_specs=[vmem] * len(RESULTS),
        out_specs=(hbm,) * len(RESULTS),
        scratch_shapes=[dma((len(RESULTS),))],
    )(*(pltpu.with_memory_space_constraint(a, pltpu.VMEM) for a in results))
    return output, new_c.reshape(state_c.shape), new_n, new_m.T


def solution(mesh):
    in_specs = (
        P("ep", None),
        P(),
        P(None, "tp"),
        P(None, "tp"),
        P(None, "tp"),
        P(),
        P(),
        P(),
        P(),
        P("ep", "tp", None, None),
        P("ep", "tp", None),
        P("ep", "tp"),
        P("tp", None),
        P(),
        P("ep", None),
        P("ep", None),
        P("ep", None, "tp"),
        P("ep", None, "tp"),
        P("ep", "tp", None),
        P(None, "tp"),
        P(None, "tp"),
        P("tp", None),
        P(),
    )
    out_specs = (P("ep", "tp"), P("ep", "tp", None, None), P("ep", "tp", None), P("ep", "tp"))
    return jax.shard_map(local, mesh=mesh, in_specs=in_specs, out_specs=out_specs, check_vma=False)
```
